32 devices in a mesh: sp: 8 (over z, y), tp: 4 (over x, core).
Axes of the slice: x: 2, y: 2, z: 4, core: 2. Of those that a mesh axis runs over, the one named last changes fastest.
Arguments:
- mixer_input: bfloat16 [4096, 1024], P('sp', 'tp'), may hold values from -6 to 6
- residual: bfloat16 [4096, 2048], P(('sp', 'tp')), may hold values from -6 to 6
- decay_real: float32 [64, 64], P('tp'), may hold values from -0.07 to 0
- decay_imag: float32 [64, 64], P('tp'), may hold values from 0.3 to 3
- log_step: float32 [64], P('tp'), may hold values from -0.7 to 0.7
- input_re: float32 [64, 64, 16], P('tp'), may hold values from -1.5 to 1.5
- input_im: float32 [64, 64, 16], P('tp'), may hold values from -1.5 to 1.5
- output_re: float32 [64, 16, 64], P('tp'), may hold values from -0.5 to 0.5
- output_im: float32 [64, 16, 64], P('tp'), may hold values from -0.5 to 0.5
- skip_gain: float32 [64, 16], P('tp'), may hold values from -4 to 4
- glu_weight: bfloat16 [1024, 1024], replicated, may hold values from -0.1875 to 0.1875
- glu_bias: float32 [1024], replicated, may hold values from -4 to 4
- mix_gain: float32 [1024], replicated, may hold values from 0.1 to 1.9
- out_weight: bfloat16 [1024, 2048], replicated, may hold values from -0.1875 to 0.1875
- norm_gain: float32 [2048], replicated, may hold values from 0.1 to 1.9
- route_ids: int32 [4096, 4], P(('sp', 'tp')), may hold values from 0 to 31, all different within a row; in each aligned block of 128 rows (0 to 127, 128 to 255, ...) at most 24 rows name the same one
- route_gates: float32 [4096, 4], P(('sp', 'tp')), may hold values from 0.25 to 1
- expert_gate: bfloat16 [32, 2048, 512], P(('sp', 'tp')), may hold values from -0.125 to 0.125
- expert_up: bfloat16 [32, 2048, 512], P(('sp', 'tp')), may hold values from -0.125 to 0.125
- expert_down: bfloat16 [32, 512, 2048], P(('sp', 'tp')), may hold values from -0.25 to 0.25
- shared_gate: bfloat16 [2048, 512], replicated, may hold values from -0.125 to 0.125
- shared_up: bfloat16 [2048, 512], replicated, may hold values from -0.125 to 0.125
- shared_down: bfloat16 [512, 2048], replicated, may hold values from -0.25 to 0.25
Outputs:
- layer_out: bfloat16 [4096, 2048], P(('sp', 'tp'))
The draws below stay inside these ranges and needn't reach their ends.
Inputs may be any that keep to these rules, and one draw needn't show every extreme that they name: `route_ids`: each row names 4 different experts; among the 128 rows of one device no expert is named by more than 24 rows, and in every draw some expert is named by exactly 24 of them.
All inputs are finite; a program needn't handle non-finite values.
Results may differ from the reference program's by a relative error of at most 0.018.
Values may be sent and summed in bfloat16 or wider, within the bound.
A program may use at most 128 MiB of HBM per device.

```python
import math
import jax
import jax.numpy as jnp
import numpy as np
from jax import lax

D = 2048
GROUPS = 64
CH = 16
STATE = 64
FF = 512
TOPK = 4
TOK_SP = 512
WIDTH = 1024
TOKENS = 4096
ROWS = 128
EXPERTS = 32
CAP = 24
N_SP = 8


def slow_groups(key, slow_share):
    return jax.random.uniform(jax.random.fold_in(key, 101), (GROUPS,)) < slow_share


def input_part(key, salt_value, slow_share):
    is_slow = slow_groups(key, slow_share)
    values = jnp.clip(jax.random.normal(jax.random.fold_in(key, salt_value), (GROUPS, STATE, CH), jnp.float32), -6.0, 6.0)
    scaling = jnp.where(is_slow, jnp.sqrt(50.0 / TOKENS), 1.0) * (2.0 * CH) ** (-0.5)
    return values * scaling[:, None, None]


def draw_decay_real(key, part):
    slow_share = 0.5
    is_slow = slow_groups(key, slow_share)
    picked = jax.random.uniform(jax.random.fold_in(key, 1), (GROUPS, STATE), jnp.float32)
    slow_rate = jnp.exp(jnp.log(0.05) + picked * jnp.log(10.0)) / TOKENS
    fast_rate = jnp.exp(jnp.log(1.0 / 50.0) + picked * jnp.log(50.0 / 15.0))
    return -jnp.where(is_slow[:, None], slow_rate, fast_rate)


def draw_input_re(key, part):
    slow_share = 0.5
    return input_part(key, 3, slow_share)


def draw_input_im(key, part):
    slow_share = 0.5
    return input_part(key, 4, slow_share)


def shard_levels(rng, extent, pieces, low, top_value):
    level = 1.0
    for dim, blocks in pieces:
        steps = jax.random.uniform(jax.random.fold_in(jax.random.fold_in(rng, 6), dim), (blocks,), jnp.float32, low / len(pieces), top_value / len(pieces))
        level = level * jnp.repeat(jnp.exp(steps), extent[dim] // blocks).reshape((-1,) + (1,) * (len(extent) - 1 - dim))
    return level


def deal_out(own_key, own, number, rows, number_of, top, reach, skew):
    order = jax.random.permutation(own_key, number_of)
    heavy_load, common = shares(number_of, rows * top, reach, skew, True), shares(number_of, rows * top, reach, skew, False)
    places = jnp.arange(number_of)

    def named(tallies, rotation):
        used = int((tallies > 0).sum())
        fixed = max(1, used // 4)
        shifted = fixed + (places - fixed + rotation * (used - fixed)) % max(1, number_of - fixed)
        return jnp.zeros((number_of,), jnp.int32).at[order[jnp.where(places < fixed, places, shifted)]].set(jnp.asarray(tallies, jnp.int32))

    tallies = jnp.where(number % 4 == 0, named(heavy_load, number // 4), named(common, number - number // 4 - 1))
    mixed = jax.random.permutation(jax.random.fold_in(own, 3), number_of)
    giver, sink = mixed[0:number_of // 2 * 2:2], mixed[1:number_of // 2 * 2:2]
    slack = jnp.minimum(tallies[giver] - 1, reach - tallies[sink]) // 2
    slack = jnp.where((giver == order[0]) | (sink == order[0]) | (tallies[sink] == 0), 0, jnp.maximum(slack, 0))
    shifted = jax.random.randint(jax.random.fold_in(own, 4), (number_of // 2,), 0, 1 << 20) % (slack + 1)
    tallies = tallies.at[giver].add(-shifted).at[sink].add(shifted)
    labels = jnp.searchsorted(jnp.cumsum(tallies), jnp.arange(rows * top), side="right").astype(jnp.int32)
    table = labels.reshape(top, rows).T
    table = table[jax.random.permutation(jax.random.fold_in(own, 1), rows)]
    rotation = jax.random.randint(jax.random.fold_in(own, 2), (rows, 1), 0, top)
    return jnp.take_along_axis(table, (jnp.arange(top)[None, :] + rotation) % top, axis=1)


def shares(number_of, total, limit, skew, full):
    portions = [(1 << 20) // math.isqrt(grade ** skew) + 1 for grade in range(1, number_of + 1)]
    largest = limit if full else min(limit, max(-(-total // number_of), total * portions[0] // sum(portions)))
    least = 1 if total - largest >= number_of - 1 else 0
    counts, spare = [largest] + [least] * (number_of - 1), total - largest - least * (number_of - 1)
    while spare > 0:
        movable = [i for i in range(1, number_of) if counts[i] < largest] or [i for i in range(1, number_of) if counts[i] < limit]
        mass, left = sum([portions[i] for i in movable]), spare
        for i in movable:
            extra = min(limit - counts[i], max(1, left * portions[i] // mass), spare)
            counts[i] = counts[i] + extra
            spare = spare - extra
    return np.array(counts)


def bell_draw(rng, extent, scale, reach, pieces=(), held_as=jnp.bfloat16):
    entries = scale * jax.random.normal(rng, extent, jnp.float32)
    if pieces:
        entries = entries * shard_levels(rng, extent, pieces, -0.22, 0.18)
    return jnp.clip(entries, -reach, reach).astype(held_as)


def setup_inputs(seed: int = 0) -> dict:
    seeds = jax.random.split(jax.random.key(seed), 24)
    mixer_input = bell_draw(seeds[0], (TOKENS, WIDTH), 1.0, 6.0, ((0, 8), (1, 4)))
    residual = bell_draw(seeds[1], (TOKENS, D), 1.0, 6.0, ((0, 32),))
    decay_real = draw_decay_real(jax.random.fold_in(seeds[23], 71), 0)
    decay_imag = jnp.clip(0.3 + 2.7 * jax.random.uniform(seeds[3], (GROUPS, STATE), jnp.float32) ** shard_levels(seeds[3], (GROUPS, STATE), ((0, 4),), -0.2, 0.2), 0.3, 3.0)
    log_step = jnp.clip(jax.random.uniform(seeds[4], (GROUPS,), jnp.float32, -0.7, 0.7) * shard_levels(seeds[4], (GROUPS,), ((0, 4),), -0.4, 0.0), -0.7, 0.7)
    input_re = draw_input_re(jax.random.fold_in(seeds[23], 71), 0)
    input_im = draw_input_im(jax.random.fold_in(seeds[23], 71), 0)
    output_re = bell_draw(seeds[7], (GROUPS, CH, STATE), (2 * STATE) ** -0.5, 0.5, ((0, 4),), jnp.float32)
    output_im = bell_draw(seeds[8], (GROUPS, CH, STATE), (2 * STATE) ** -0.5, 0.5, ((0, 4),), jnp.float32)
    skip_gain = bell_draw(seeds[9], (GROUPS, CH), 1.0, 4.0, ((0, 4),), jnp.float32)
    glu_weight = bell_draw(seeds[10], (WIDTH, WIDTH), WIDTH ** -0.5, 0.1875)
    glu_bias = bell_draw(seeds[11], (WIDTH,), 1.0, 4.0, (), jnp.float32)
    mix_gain = jnp.clip(1.0 + 0.18 * jax.random.normal(seeds[12], (WIDTH,), jnp.float32), 0.1, 1.9)
    out_weight = bell_draw(seeds[13], (WIDTH, D), WIDTH ** -0.5, 0.1875)
    norm_gain = jnp.clip(1.0 + 0.18 * jax.random.normal(seeds[14], (D,), jnp.float32), 0.1, 1.9)
    route_ids_keys = jax.random.split(jax.random.fold_in(seeds[15], 1), TOKENS // ROWS)
    route_ids_turns = jax.random.permutation(jax.random.fold_in(seeds[15], 3), TOKENS // ROWS)
    route_ids = jax.vmap(lambda own, number: deal_out(jax.random.fold_in(seeds[15], 2), own, number, ROWS, EXPERTS, TOPK, CAP, 2))(route_ids_keys, route_ids_turns).reshape((TOKENS, TOPK))
    route_gates = jnp.clip(0.25 + 0.75 * jax.random.uniform(seeds[16], (TOKENS, TOPK), jnp.float32) ** shard_levels(seeds[16], (TOKENS, TOPK), ((0, 32),), -0.2, 0.2), 0.25, 1.0)
    expert_gate = bell_draw(seeds[17], (EXPERTS, D, FF), D ** -0.5, 0.125, ((0, 32),))
    expert_up = bell_draw(seeds[18], (EXPERTS, D, FF), D ** -0.5, 0.125, ((0, 32),))
    expert_down = bell_draw(seeds[19], (EXPERTS, FF, D), FF ** -0.5, 0.25, ((0, 32),))
    shared_gate = bell_draw(seeds[20], (D, FF), D ** -0.5, 0.125)
    shared_up = bell_draw(seeds[21], (D, FF), D ** -0.5, 0.125)
    shared_down = bell_draw(seeds[22], (FF, D), FF ** -0.5, 0.25)
    return {"mixer_input": mixer_input, "residual": residual, "decay_real": decay_real, "decay_imag": decay_imag, "log_step": log_step, "input_re": input_re, "input_im": input_im, "output_re": output_re, "output_im": output_im, "skip_gain": skip_gain, "glu_weight": glu_weight, "glu_bias": glu_bias, "mix_gain": mix_gain, "out_weight": out_weight, "norm_gain": norm_gain, "route_ids": route_ids, "route_gates": route_gates, "expert_gate": expert_gate, "expert_up": expert_up, "expert_down": expert_down, "shared_gate": shared_gate, "shared_up": shared_up, "shared_down": shared_down}


NORM_EPS = 1e-06
HIGHEST = lax.Precision.HIGHEST

def discretize(decay_real, decay_imag, log_step, input_re, input_im):
    step_size = jnp.exp(log_step)[:, None]
    log_rate = decay_real * step_size
    turn_angle = decay_imag * step_size
    bar_re = jnp.exp(log_rate) * jnp.cos(turn_angle)
    bar_im = jnp.exp(log_rate) * jnp.sin(turn_angle)
    denominator = decay_real * decay_real + decay_imag * decay_imag
    less_one = bar_re - 1.0
    coef_re = (less_one * decay_real + bar_im * decay_imag) / denominator
    coef_im = (bar_im * decay_real - less_one * decay_imag) / denominator
    drive_re = coef_re[:, :, None] * input_re - coef_im[:, :, None] * input_im
    drive_im = coef_re[:, :, None] * input_im + coef_im[:, :, None] * input_re
    return (log_rate.reshape(-1), turn_angle.reshape(-1), jnp.concatenate([drive_re, drive_im], axis=1))

def powers(count, log_rate, turn_angle):
    magnitude = jnp.exp(count * log_rate)
    return (magnitude * jnp.cos(count * turn_angle), magnitude * jnp.sin(count * turn_angle))

def local_states(inputs, drive, log_rate, turn_angle):
    length, width_all = inputs.shape
    group_count = drive.shape[0]
    channels = width_all // group_count
    state_count = drive.shape[1] // 2
    driven = jnp.einsum('lgc,gnc->lgn', inputs.astype(jnp.float32).reshape(length, group_count, channels), drive, precision=HIGHEST)
    state_re = driven[:, :, :state_count].reshape(length, group_count * state_count)
    state_im = driven[:, :, state_count:].reshape(length, group_count * state_count)
    offset = 1
    while offset < length:
        pow_re, pow_im = powers(float(offset), log_rate, turn_angle)
        prior_re = jnp.pad(state_re[:-offset], ((offset, 0), (0, 0)))
        prior_im = jnp.pad(state_im[:-offset], ((offset, 0), (0, 0)))
        state_re, state_im = (state_re + pow_re * prior_re - pow_im * prior_im, state_im + pow_re * prior_im + pow_im * prior_re)
        offset *= 2
    return (state_re, state_im)

def read_out(state_re, state_im, output_re, output_im):
    length = state_re.shape[0]
    group_count, channels, state_count = output_re.shape
    stacked = jnp.concatenate([state_re.reshape(length, group_count, state_count), state_im.reshape(length, group_count, state_count)], axis=2)
    table = jnp.concatenate([output_re, -output_im], axis=2)
    return jnp.einsum('lgn,gcn->lgc', stacked, table, precision=HIGHEST).reshape(length, group_count * channels)

def rms_scale(values, gain):
    return values * lax.rsqrt(lax.optimization_barrier(jnp.mean(values * values, axis=-1, keepdims=True)) + NORM_EPS) * gain

def reference(mixer_input, residual, decay_real, decay_imag, log_step, input_re, input_im, output_re, output_im, skip_gain, glu_weight, glu_bias, mix_gain, out_weight, norm_gain, route_ids, route_gates, expert_gate, expert_up, expert_down, shared_gate, shared_up, shared_down):
    log_rate, turn_angle, drive = discretize(decay_real, decay_imag, log_step, input_re, input_im)
    blocks = mixer_input.reshape(N_SP, TOK_SP, WIDTH)
    positions = jnp.arange(1, TOK_SP + 1, dtype=jnp.float32)[:, None]
    pow_re, pow_im = powers(positions, log_rate, turn_angle)

    def advance(carry_state, block_input):
        state_re, state_im = local_states(block_input, drive, log_rate, turn_angle)
        full_re = state_re + pow_re * carry_state[0] - pow_im * carry_state[1]
        full_im = state_im + pow_re * carry_state[1] + pow_im * carry_state[0]
        readout = read_out(full_re, full_im, output_re, output_im)
        mixed = jax.nn.gelu(readout + skip_gain.reshape(-1) * block_input.astype(jnp.float32))
        return ((full_re[-1], full_im[-1]), mixed.astype(jnp.bfloat16))
    start = (jnp.zeros_like(log_rate), jnp.zeros_like(log_rate))
    mixed = lax.scan(advance, start, blocks)[1].reshape(TOKENS, WIDTH)
    pre_gate = jnp.dot(mixed, glu_weight, preferred_element_type=jnp.float32) + glu_bias
    gated = mixed.astype(jnp.float32) * jax.nn.sigmoid(pre_gate)
    normed = rms_scale(gated, mix_gain).astype(jnp.bfloat16)
    stream = residual.astype(jnp.float32) + jnp.dot(normed, out_weight, preferred_element_type=jnp.float32)
    hidden_in = rms_scale(stream, norm_gain).astype(jnp.bfloat16)
    shared_hidden = (jax.nn.silu(jnp.dot(hidden_in, shared_gate, preferred_element_type=jnp.float32)) * jnp.dot(hidden_in, shared_up, preferred_element_type=jnp.float32)).astype(jnp.bfloat16)
    total = stream + jnp.dot(shared_hidden, shared_down, preferred_element_type=jnp.float32)
    flat_ids = route_ids.reshape(-1)
    flat_gates = route_gates.reshape(-1)
    slot_count = EXPERTS * CAP

    def one_expert(routed, expert):
        missing = (flat_ids != expert).astype(jnp.int32)
        ordering = jnp.argsort(missing, stable=True)[:slot_count].astype(jnp.int32)
        is_valid = flat_ids[ordering] == expert
        token_idx = (ordering // TOPK).astype(jnp.int32)
        rows_in = hidden_in[token_idx]
        gate_w = lax.dynamic_index_in_dim(expert_gate, expert, 0, keepdims=False)
        up_w = lax.dynamic_index_in_dim(expert_up, expert, 0, keepdims=False)
        down_w = lax.dynamic_index_in_dim(expert_down, expert, 0, keepdims=False)
        hidden = (jax.nn.silu(jnp.dot(rows_in, gate_w, preferred_element_type=jnp.float32)) * jnp.dot(rows_in, up_w, preferred_element_type=jnp.float32)).astype(jnp.bfloat16)
        expert_out = jnp.dot(hidden, down_w, preferred_element_type=jnp.float32).astype(jnp.bfloat16)
        weight = jnp.where(is_valid, flat_gates[ordering], jnp.zeros_like(flat_gates[ordering]))
        return (routed.at[token_idx].add(weight[:, None] * expert_out.astype(jnp.float32)), None)
    routed = lax.scan(one_expert, jnp.zeros((TOKENS, D), jnp.float32), jnp.arange(EXPERTS, dtype=jnp.int32))[0]
    return (total + routed).astype(jnp.bfloat16)
```

```python
import functools
import math

import jax
import jax.numpy as jnp
from jax import lax
from jax.experimental import pallas as pl
from jax.experimental.pallas import tpu as pltpu
from jax.sharding import PartitionSpec as P

NORM_EPS = 1e-06
HIGHEST = lax.Precision.HIGHEST
MESH = pl.DeviceIdType.MESH


def exchange_kernel(count, position, member, same, block_ref, out_ref, send_sem, recv_sem, own_sem):
    me = position()
    barrier = pltpu.get_barrier_semaphore()

    def greet(step, carry):
        pl.semaphore_signal(
            barrier, inc=1, device_id=member(lax.rem(me + step, count)), device_id_type=MESH
        )
        return carry

    def copy(step):
        to = lax.rem(me + step, count)
        return pltpu.make_async_remote_copy(
            src_ref=block_ref if same else block_ref.at[to],
            dst_ref=out_ref.at[me],
            send_sem=send_sem.at[step],
            recv_sem=recv_sem.at[step],
            device_id=member(to),
            device_id_type=MESH,
        )

    def begin(step, carry):
        copy(step).start()
        return carry

    def finish(step, carry):
        copy(step).wait()
        return carry

    own = pltpu.make_async_copy(block_ref if same else block_ref.at[me], out_ref.at[me], own_sem)
    own.start()
    lax.fori_loop(1, count, greet, 0)
    pl.semaphore_wait(barrier, count - 1)
    lax.fori_loop(1, count, begin, 0)
    lax.fori_loop(1, count, finish, 0)
    own.wait()


def exchange(block, count, position, member, collective_id, same=False):
    shape = (count,) + block.shape if same else block.shape
    return pl.pallas_call(
        functools.partial(exchange_kernel, count, position, member, same),
        out_shape=jax.ShapeDtypeStruct(shape, block.dtype),
        in_specs=[pl.BlockSpec(memory_space=pl.ANY)],
        out_specs=pl.BlockSpec(memory_space=pl.ANY),
        scratch_shapes=[
            pltpu.SemaphoreType.DMA((count,)),
            pltpu.SemaphoreType.DMA((count,)),
            pltpu.SemaphoreType.DMA,
        ],
        compiler_params=pltpu.CompilerParams(collective_id=collective_id, has_side_effects=True),
    )(block)


def gather_sp(block):
    return exchange(
        block,
        lax.axis_size("sp"),
        lambda: lax.axis_index("sp"),
        lambda index: (index, lax.axis_index("tp")),
        1,
        same=True,
    )


def exchange_tp(block):
    return exchange(
        block,
        lax.axis_size("tp"),
        lambda: lax.axis_index("tp"),
        lambda index: (lax.axis_index("sp"), index),
        2,
    )


def exchange_all(block, collective_id):
    width = lax.axis_size("tp")
    return exchange(
        block,
        lax.axis_size(("sp", "tp")),
        lambda: lax.axis_index("sp") * width + lax.axis_index("tp"),
        lambda index: (index // width, lax.rem(index, width)),
        collective_id,
    )


CHUNK = 16


def times(a, b):
    return (a[0] * b[0] - a[1] * b[1], a[0] * b[1] + a[1] * b[0])


def mixer(inputs, decay_real, decay_imag, log_step, input_re, input_im, output_re, output_im, skip):
    length = inputs.shape[0]
    groups, states, channels = input_re.shape
    chunks = length // CHUNK
    step_size = jnp.exp(log_step)[:, None]
    log_rate = decay_real * step_size
    turn_angle = decay_imag * step_size

    def powers(count):
        magnitude = jnp.exp(count * log_rate)
        return (magnitude * jnp.cos(count * turn_angle), magnitude * jnp.sin(count * turn_angle))

    bar_re, bar_im = powers(1.0)
    denominator = decay_real * decay_real + decay_imag * decay_imag
    less_one = bar_re - 1.0
    coef = (
        (less_one * decay_real + bar_im * decay_imag) / denominator,
        (bar_im * decay_real - less_one * decay_imag) / denominator,
    )
    drive = times((coef[0][:, :, None], coef[1][:, :, None]), (input_re, input_im))
    steps = jnp.arange(1, CHUNK + 1, dtype=jnp.float32)
    ahead = powers(steps[:, None, None])
    ahead = tuple(jnp.swapaxes(part, 0, 1)[:, :, None, :] for part in ahead)
    reads = times(ahead, (output_re[:, None], output_im[:, None]))
    reads = jnp.concatenate([reads[0], -reads[1]], axis=3).reshape(
        groups, CHUNK * channels, 2 * states
    )
    back = powers(-steps[:, None, None])
    back = tuple(jnp.swapaxes(part, 0, 1)[:, :, None, :] for part in back)
    drive = tuple(jnp.swapaxes(part, 1, 2)[:, None] for part in drive)
    feeds = times(back, drive)
    feeds = jnp.concatenate(feeds, axis=3).reshape(groups, CHUNK * channels, 2 * states)
    rows = jnp.arange(CHUNK * channels, dtype=jnp.int32) // channels
    kernel = jnp.einsum("gsn,gtn->gst", feeds, reads, precision=HIGHEST)
    kernel = jnp.where(rows[:, None] <= rows[None, :], kernel, 0.0)
    wide = (
        inputs.reshape(chunks, CHUNK, groups, channels)
        .transpose(2, 0, 1, 3)
        .reshape(groups, chunks, CHUNK * channels)
        .astype(jnp.float32)
    )
    local = jnp.einsum("gks,gst->gkt", wide, kernel, precision=HIGHEST)
    driven = jnp.einsum("gks,gsn->gkn", wide, feeds, precision=HIGHEST)
    whole = tuple(part[:, None] for part in powers(float(CHUNK)))
    state = times(whole, (driven[:, :, :states], driven[:, :, states:]))
    offset = 1
    while offset < chunks:
        prior = tuple(
            jnp.pad(part[:, :-offset], ((0, 0), (offset, 0), (0, 0))) for part in state
        )
        moved = times(tuple(part[:, None] for part in powers(float(CHUNK * offset))), prior)
        state = (state[0] + moved[0], state[1] + moved[1])
        offset *= 2
    ends = jnp.concatenate([state[0][:, -1], state[1][:, -1]], axis=1)
    ends = ends.reshape(groups * states * 2 // 128, 128)
    pieces = gather_sp(ends).reshape(-1, groups, 2 * states)
    my_index = lax.axis_index("sp")
    sources = jnp.arange(pieces.shape[0], dtype=jnp.int32)
    earlier = sources < my_index
    distance = jnp.where(earlier, my_index - 1 - sources, 0).astype(jnp.float32)[:, None, None]
    weight = jnp.where(earlier, 1.0, 0.0).astype(jnp.float32)[:, None, None]
    block_angle = jnp.mod(float(length) * turn_angle, 2.0 * math.pi)
    magnitude = jnp.exp(distance * (float(length) * log_rate)) * weight
    factor = (
        magnitude * jnp.cos(distance * block_angle),
        magnitude * jnp.sin(distance * block_angle),
    )
    added = times(factor, (pieces[:, :, :states], pieces[:, :, states:]))
    carried = tuple(jnp.sum(part, axis=0)[:, None] for part in added)
    starts = powers(float(CHUNK) * jnp.arange(chunks, dtype=jnp.float32)[:, None, None])
    starts = tuple(jnp.swapaxes(part, 0, 1) for part in starts)
    carried = times(starts, carried)
    before = jnp.concatenate(
        [
            jnp.pad(state[i][:, :-1], ((0, 0), (1, 0), (0, 0))) + carried[i]
            for i in range(2)
        ],
        axis=2,
    )
    readout = local + jnp.einsum("gkn,gtn->gkt", before, reads, precision=HIGHEST)
    gains = jnp.broadcast_to(skip[:, None, :], (groups, CHUNK, channels))
    mixed = jax.nn.gelu(readout + gains.reshape(groups, 1, -1) * wide).astype(jnp.bfloat16)
    return (
        mixed.reshape(groups, chunks, CHUNK, channels)
        .transpose(1, 2, 0, 3)
        .reshape(length, groups * channels)
    )


def rms_scale(values, gain):
    return values * lax.rsqrt(jnp.mean(values * values, axis=-1, keepdims=True) + NORM_EPS) * gain


def earlier_rows(onehot):
    count = onehot.shape[0]
    lower = jnp.tril(jnp.ones((count, count), jnp.bfloat16))
    return jnp.dot(lower, onehot.astype(jnp.bfloat16), preferred_element_type=jnp.float32)


def expert_apply(arrived, gate_w, up_w, down_w):
    block_shape = arrived.shape
    flattened = arrived.reshape(-1, block_shape[-1])
    hidden = (
        jax.nn.silu(jnp.dot(flattened, gate_w, preferred_element_type=jnp.float32))
        * jnp.dot(flattened, up_w, preferred_element_type=jnp.float32)
    ).astype(jnp.bfloat16)
    result = jnp.dot(hidden, down_w, preferred_element_type=jnp.float32).astype(jnp.bfloat16)
    return result.reshape(block_shape)


def on_device(
    mixer_input,
    residual,
    decay_real,
    decay_imag,
    log_step,
    input_re,
    input_im,
    output_re,
    output_im,
    skip_gain,
    glu_weight,
    glu_bias,
    mix_gain,
    out_weight,
    norm_gain,
    route_ids,
    route_gates,
    expert_gate,
    expert_up,
    expert_down,
    shared_gate,
    shared_up,
    shared_down,
):
    mixed = mixer(
        mixer_input,
        decay_real,
        decay_imag,
        log_step,
        input_re,
        input_im,
        output_re,
        output_im,
        skip_gain,
    )
    tp_count = lax.axis_size("tp")
    token_rows = exchange_tp(mixed.reshape(tp_count, -1, mixed.shape[1]))
    token_rows = token_rows.transpose(1, 0, 2).reshape(token_rows.shape[1], -1)
    pre_gate = jnp.dot(token_rows, glu_weight, preferred_element_type=jnp.float32) + glu_bias
    gated = token_rows.astype(jnp.float32) * jax.nn.sigmoid(pre_gate)
    normed = rms_scale(gated, mix_gain).astype(jnp.bfloat16)
    stream = residual.astype(jnp.float32) + jnp.dot(
        normed, out_weight, preferred_element_type=jnp.float32
    )
    hidden_in = rms_scale(stream, norm_gain).astype(jnp.bfloat16)
    shared_hidden = (
        jax.nn.silu(jnp.dot(hidden_in, shared_gate, preferred_element_type=jnp.float32))
        * jnp.dot(hidden_in, shared_up, preferred_element_type=jnp.float32)
    ).astype(jnp.bfloat16)
    total = stream + jnp.dot(shared_hidden, shared_down, preferred_element_type=jnp.float32)
    row_count, top_count = route_ids.shape
    model_width = hidden_in.shape[1]
    expert_count = lax.axis_size(("sp", "tp"))
    capacity = max(2, 3 * row_count * top_count // (2 * expert_count))
    flat_ids = route_ids.reshape(-1)
    onehot = (flat_ids[:, None] == jnp.arange(expert_count, dtype=jnp.int32)[None, :]).astype(
        jnp.float32
    )
    ranks = jnp.sum((earlier_rows(onehot) - onehot) * onehot, axis=1)
    slots = (flat_ids * capacity + ranks.astype(jnp.int32)).reshape(row_count, top_count)
    slot_numbers = jnp.arange(expert_count * capacity, dtype=jnp.int32)
    hits = [slots[:, index : index + 1] == slot_numbers for index in range(top_count)]
    placed = functools.reduce(jnp.logical_or, hits).astype(jnp.bfloat16)
    outgoing = (
        lax.dot_general(
            placed, hidden_in, (((0,), (0,)), ((), ())), preferred_element_type=jnp.float32
        )
        .astype(jnp.bfloat16)
        .reshape(expert_count, capacity, model_width)
    )
    gates = sum(
        jnp.where(hits[index], route_gates[:, index : index + 1], 0.0)
        for index in range(top_count)
    )
    coarse = gates.astype(jnp.bfloat16)
    fine = (gates - coarse.astype(jnp.float32)).astype(jnp.bfloat16)
    gate_w = expert_gate[0]
    up_w = expert_up[0]
    down_w = expert_down[0]
    returned = exchange_all(
        expert_apply(exchange_all(outgoing, 3), gate_w, up_w, down_w), 4
    )
    rows = returned.reshape(expert_count * capacity, model_width)
    total = (
        total
        + jnp.dot(coarse, rows, preferred_element_type=jnp.float32)
        + jnp.dot(fine, rows, preferred_element_type=jnp.float32)
    )
    return total.astype(jnp.bfloat16)


def solution(mesh):
    return jax.shard_map(
        on_device,
        mesh=mesh,
        in_specs=(
            P("sp", "tp"),
            P(("sp", "tp"), None),
            P("tp", None),
            P("tp", None),
            P("tp"),
            P("tp", None, None),
            P("tp", None, None),
            P("tp", None, None),
            P("tp", None, None),
            P("tp", None),
            P(),
            P(),
            P(),
            P(),
            P(),
            P(("sp", "tp"), None),
            P(("sp", "tp"), None),
            P(("sp", "tp"), None, None),
            P(("sp", "tp"), None, None),
            P(("sp", "tp"), None, None),
            P(),
            P(),
            P(),
        ),
        out_specs=P(("sp", "tp"), None),
        check_vma=False,
    )
```

```python
import functools
import math

import jax
import jax.numpy as jnp
from jax import lax
from jax.experimental import pallas as pl
from jax.experimental.pallas import tpu as pltpu
from jax.sharding import PartitionSpec as P

NORM_EPS = 1e-06
HIGHEST = lax.Precision.HIGHEST
MESH = pl.DeviceIdType.MESH


def exchange_kernel(count, position, member, same, block_ref, out_ref, send_sem, recv_sem, own_sem):
    me = position()
    barrier = pltpu.get_barrier_semaphore()

    def greet(step, carry):
        pl.semaphore_signal(
            barrier, inc=1, device_id=member(lax.rem(me + step, count)), device_id_type=MESH
        )
        return carry

    stride = 7 if math.gcd(7, count - 1) == 1 else 1

    def copy(step):
        ahead = 1 + lax.rem((step - 1) * stride + count // 4, count - 1)
        to = lax.rem(me + ahead, count)
        return pltpu.make_async_remote_copy(
            src_ref=block_ref if same else block_ref.at[to],
            dst_ref=out_ref.at[me],
            send_sem=send_sem.at[step],
            recv_sem=recv_sem.at[step],
            device_id=member(to),
            device_id_type=MESH,
        )

    def begin(step, carry):
        copy(step).start()
        return carry

    def finish(step, carry):
        copy(step).wait()
        return carry

    own = pltpu.make_async_copy(block_ref if same else block_ref.at[me], out_ref.at[me], own_sem)
    own.start()
    lax.fori_loop(1, count, greet, 0)
    pl.semaphore_wait(barrier, count - 1)
    lax.fori_loop(1, count, begin, 0)
    lax.fori_loop(1, count, finish, 0)
    own.wait()


def exchange(block, count, position, member, collective_id, same=False):
    shape = (count,) + block.shape if same else block.shape
    return pl.pallas_call(
        functools.partial(exchange_kernel, count, position, member, same),
        out_shape=jax.ShapeDtypeStruct(shape, block.dtype),
        in_specs=[pl.BlockSpec(memory_space=pl.ANY)],
        out_specs=pl.BlockSpec(memory_space=pl.ANY),
        scratch_shapes=[
            pltpu.SemaphoreType.DMA((count,)),
            pltpu.SemaphoreType.DMA((count,)),
            pltpu.SemaphoreType.DMA,
        ],
        compiler_params=pltpu.CompilerParams(collective_id=collective_id, has_side_effects=True),
    )(block)


def gather_sp(block):
    return exchange(
        block,
        lax.axis_size("sp"),
        lambda: lax.axis_index("sp"),
        lambda index: (index, lax.axis_index("tp")),
        1,
        same=True,
    )


def exchange_tp(block):
    return exchange(
        block,
        lax.axis_size("tp"),
        lambda: lax.axis_index("tp"),
        lambda index: (lax.axis_index("sp"), index),
        2,
    )


def exchange_all(block, collective_id):
    width = lax.axis_size("tp")
    return exchange(
        block,
        lax.axis_size(("sp", "tp")),
        lambda: lax.axis_index("sp") * width + lax.axis_index("tp"),
        lambda index: (index // width, lax.rem(index, width)),
        collective_id,
    )


CHUNK = 16


def times(a, b):
    return (a[0] * b[0] - a[1] * b[1], a[0] * b[1] + a[1] * b[0])


def mixer(inputs, decay_real, decay_imag, log_step, input_re, input_im, output_re, output_im, skip):
    length = inputs.shape[0]
    groups, states, channels = input_re.shape
    chunks = length // CHUNK
    step_size = jnp.exp(log_step)[:, None]
    log_rate = decay_real * step_size
    turn_angle = decay_imag * step_size

    def powers(count):
        magnitude = jnp.exp(count * log_rate)
        return (magnitude * jnp.cos(count * turn_angle), magnitude * jnp.sin(count * turn_angle))

    bar_re, bar_im = powers(1.0)
    denominator = decay_real * decay_real + decay_imag * decay_imag
    less_one = bar_re - 1.0
    coef = (
        (less_one * decay_real + bar_im * decay_imag) / denominator,
        (bar_im * decay_real - less_one * decay_imag) / denominator,
    )
    drive = times((coef[0][:, :, None], coef[1][:, :, None]), (input_re, input_im))
    steps = jnp.arange(1, CHUNK + 1, dtype=jnp.float32)
    ahead = powers(steps[:, None, None])
    ahead = tuple(jnp.swapaxes(part, 0, 1)[:, :, None, :] for part in ahead)
    reads = times(ahead, (output_re[:, None], output_im[:, None]))
    reads = jnp.concatenate([reads[0], -reads[1]], axis=3).reshape(
        groups, CHUNK * channels, 2 * states
    )
    back = powers(-steps[:, None, None])
    back = tuple(jnp.swapaxes(part, 0, 1)[:, :, None, :] for part in back)
    drive = tuple(jnp.swapaxes(part, 1, 2)[:, None] for part in drive)
    feeds = times(back, drive)
    feeds = jnp.concatenate(feeds, axis=3).reshape(groups, CHUNK * channels, 2 * states)
    rows = jnp.arange(CHUNK * channels, dtype=jnp.int32) // channels
    kernel = jnp.einsum("gsn,gtn->gst", feeds, reads, precision=HIGHEST)
    kernel = jnp.where(rows[:, None] <= rows[None, :], kernel, 0.0)
    wide = (
        inputs.reshape(chunks, CHUNK, groups, channels)
        .transpose(2, 0, 1, 3)
        .reshape(groups, chunks, CHUNK * channels)
        .astype(jnp.float32)
    )
    local = jnp.einsum("gks,gst->gkt", wide, kernel, precision=HIGHEST)
    driven = jnp.einsum("gks,gsn->gkn", wide, feeds, precision=HIGHEST)
    whole = tuple(part[:, None] for part in powers(float(CHUNK)))
    state = times(whole, (driven[:, :, :states], driven[:, :, states:]))
    offset = 1
    while offset < chunks:
        prior = tuple(
            jnp.pad(part[:, :-offset], ((0, 0), (offset, 0), (0, 0))) for part in state
        )
        moved = times(tuple(part[:, None] for part in powers(float(CHUNK * offset))), prior)
        state = (state[0] + moved[0], state[1] + moved[1])
        offset *= 2
    ends = jnp.concatenate([state[0][:, -1], state[1][:, -1]], axis=1)
    ends = ends.reshape(groups * states * 2 // 128, 128)
    pieces = gather_sp(ends).reshape(-1, groups, 2 * states)
    my_index = lax.axis_index("sp")
    sources = jnp.arange(pieces.shape[0], dtype=jnp.int32)
    earlier = sources < my_index
    distance = jnp.where(earlier, my_index - 1 - sources, 0).astype(jnp.float32)[:, None, None]
    weight = jnp.where(earlier, 1.0, 0.0).astype(jnp.float32)[:, None, None]
    block_angle = jnp.mod(float(length) * turn_angle, 2.0 * math.pi)
    magnitude = jnp.exp(distance * (float(length) * log_rate)) * weight
    factor = (
        magnitude * jnp.cos(distance * block_angle),
        magnitude * jnp.sin(distance * block_angle),
    )
    added = times(factor, (pieces[:, :, :states], pieces[:, :, states:]))
    carried = tuple(jnp.sum(part, axis=0)[:, None] for part in added)
    starts = powers(float(CHUNK) * jnp.arange(chunks, dtype=jnp.float32)[:, None, None])
    starts = tuple(jnp.swapaxes(part, 0, 1) for part in starts)
    carried = times(starts, carried)
    before = jnp.concatenate(
        [
            jnp.pad(state[i][:, :-1], ((0, 0), (1, 0), (0, 0))) + carried[i]
            for i in range(2)
        ],
        axis=2,
    )
    readout = local + jnp.einsum("gkn,gtn->gkt", before, reads, precision=HIGHEST)
    gains = jnp.broadcast_to(skip[:, None, :], (groups, CHUNK, channels))
    mixed = jax.nn.gelu(readout + gains.reshape(groups, 1, -1) * wide).astype(jnp.bfloat16)
    return (
        mixed.reshape(groups, chunks, CHUNK, channels)
        .transpose(1, 2, 0, 3)
        .reshape(length, groups * channels)
    )


def rms_scale(values, gain):
    return values * lax.rsqrt(jnp.mean(values * values, axis=-1, keepdims=True) + NORM_EPS) * gain


def earlier_rows(onehot):
    count = onehot.shape[0]
    lower = jnp.tril(jnp.ones((count, count), jnp.bfloat16))
    return jnp.dot(lower, onehot.astype(jnp.bfloat16), preferred_element_type=jnp.float32)


def expert_apply(arrived, gate_w, up_w, down_w):
    block_shape = arrived.shape
    flattened = arrived.reshape(-1, block_shape[-1])
    hidden = (
        jax.nn.silu(jnp.dot(flattened, gate_w, preferred_element_type=jnp.float32))
        * jnp.dot(flattened, up_w, preferred_element_type=jnp.float32)
    ).astype(jnp.bfloat16)
    result = jnp.dot(hidden, down_w, preferred_element_type=jnp.float32).astype(jnp.bfloat16)
    return result.reshape(block_shape)


def on_device(
    mixer_input,
    residual,
    decay_real,
    decay_imag,
    log_step,
    input_re,
    input_im,
    output_re,
    output_im,
    skip_gain,
    glu_weight,
    glu_bias,
    mix_gain,
    out_weight,
    norm_gain,
    route_ids,
    route_gates,
    expert_gate,
    expert_up,
    expert_down,
    shared_gate,
    shared_up,
    shared_down,
):
    mixed = mixer(
        mixer_input,
        decay_real,
        decay_imag,
        log_step,
        input_re,
        input_im,
        output_re,
        output_im,
        skip_gain,
    )
    tp_count = lax.axis_size("tp")
    token_rows = exchange_tp(mixed.reshape(tp_count, -1, mixed.shape[1]))
    token_rows = token_rows.transpose(1, 0, 2).reshape(token_rows.shape[1], -1)
    pre_gate = jnp.dot(token_rows, glu_weight, preferred_element_type=jnp.float32) + glu_bias
    gated = token_rows.astype(jnp.float32) * jax.nn.sigmoid(pre_gate)
    normed = rms_scale(gated, mix_gain).astype(jnp.bfloat16)
    stream = residual.astype(jnp.float32) + jnp.dot(
        normed, out_weight, preferred_element_type=jnp.float32
    )
    hidden_in = rms_scale(stream, norm_gain).astype(jnp.bfloat16)
    shared_hidden = (
        jax.nn.silu(jnp.dot(hidden_in, shared_gate, preferred_element_type=jnp.float32))
        * jnp.dot(hidden_in, shared_up, preferred_element_type=jnp.float32)
    ).astype(jnp.bfloat16)
    total = stream + jnp.dot(shared_hidden, shared_down, preferred_element_type=jnp.float32)
    row_count, top_count = route_ids.shape
    model_width = hidden_in.shape[1]
    expert_count = lax.axis_size(("sp", "tp"))
    capacity = max(2, 3 * row_count * top_count // (2 * expert_count))
    flat_ids = route_ids.reshape(-1)
    onehot = (flat_ids[:, None] == jnp.arange(expert_count, dtype=jnp.int32)[None, :]).astype(
        jnp.float32
    )
    ranks = jnp.sum((earlier_rows(onehot) - onehot) * onehot, axis=1)
    slots = (flat_ids * capacity + ranks.astype(jnp.int32)).reshape(row_count, top_count)
    slot_numbers = jnp.arange(expert_count * capacity, dtype=jnp.int32)
    hits = [slots[:, index : index + 1] == slot_numbers for index in range(top_count)]
    placed = functools.reduce(jnp.logical_or, hits).astype(jnp.bfloat16)
    outgoing = (
        lax.dot_general(
            placed, hidden_in, (((0,), (0,)), ((), ())), preferred_element_type=jnp.float32
        )
        .astype(jnp.bfloat16)
        .reshape(expert_count, capacity, model_width)
    )
    gates = sum(
        jnp.where(hits[index], route_gates[:, index : index + 1], 0.0)
        for index in range(top_count)
    )
    coarse = gates.astype(jnp.bfloat16)
    fine = (gates - coarse.astype(jnp.float32)).astype(jnp.bfloat16)
    gate_w = expert_gate[0]
    up_w = expert_up[0]
    down_w = expert_down[0]
    returned = exchange_all(
        expert_apply(exchange_all(outgoing, 3), gate_w, up_w, down_w), 4
    )
    rows = returned.reshape(expert_count * capacity, model_width)
    total = (
        total
        + jnp.dot(coarse, rows, preferred_element_type=jnp.float32)
        + jnp.dot(fine, rows, preferred_element_type=jnp.float32)
    )
    return total.astype(jnp.bfloat16)


def solution(mesh):
    return jax.shard_map(
        on_device,
        mesh=mesh,
        in_specs=(
            P("sp", "tp"),
            P(("sp", "tp"), None),
            P("tp", None),
            P("tp", None),
            P("tp"),
            P("tp", None, None),
            P("tp", None, None),
            P("tp", None, None),
            P("tp", None, None),
            P("tp", None),
            P(),
            P(),
            P(),
            P(),
            P(),
            P(("sp", "tp"), None),
            P(("sp", "tp"), None),
            P(("sp", "tp"), None, None),
            P(("sp", "tp"), None, None),
            P(("sp", "tp"), None, None),
            P(),
            P(),
            P(),
        ),
        out_specs=P(("sp", "tp"), None),
        check_vma=False,
    )
```
